768 devices in a mesh: gr: 3 (over z_hi), sp: 32 (over z_lo, y), tp: 8 (over x, core).
Axes of the slice: x: 4, y: 8, z: 12 (z_hi: 3, z_lo: 4; z = z_hi * 4 + z_lo), core: 2. Of those that a mesh axis runs over, the one named last changes fastest.
Arguments:
- tokens: bfloat16 [12, 6144, 4096], P('gr', 'sp'), parts along dimension 0, may hold values from -50 to 50
- new_tokens: bfloat16 [12, 4096], P('gr'), parts along dimension 0, may hold values from -6 to 6
- in_gain: float32 [4096], replicated, may hold values from 0.1 to 1.9
- w_forget: bfloat16 [4096, 2048], P(None, 'tp'), may hold values from -0.09375 to 0.09375
- w_value: bfloat16 [4096, 2048], P(None, 'tp'), may hold values from -0.75 to 0.75
- gap: float32 [16, 128], P('tp'), may hold values from 0 to 0.06
- decay_shift: float32 [12, 6144, 16], P('gr', 'sp', 'tp'), parts along dimension 0, may hold values from -3 to 0
- query: bfloat16 [12, 16, 128], P('gr', 'tp', 'sp'), parts along dimension 0, may hold values from -6 to 6
- out_gain: float32 [16, 128], P('tp'), may hold values from 0.1 to 1.9
Outputs:
- cache: bfloat16 [12, 16, 128, 128], P('gr', 'tp', 'sp'), parts along dimension 0
- read: float32 [12, 16, 128], P('gr', 'tp'), parts along dimension 0
The draws below stay inside these ranges and needn't reach their ends.
There are 3 independent parts, one for each index of `gr`. The reference program is written for one: setup_inputs(seed, part) draws one part's arguments, and reference() takes and returns one part's arrays. A program takes and returns all parts, laid end to end along the dimension named above; an argument that names none is the same for every part. Nothing has to cross between parts.
All inputs are finite; a program needn't handle non-finite values.
Results may differ from the reference program's by a relative error of at most 0.0065.
Values sent between devices are 32-bit elements; how exact they have to be, the bound alone decides.
No kernel may reach another device: no remote copies, remote signals or barrier semaphores. Data moves between devices by JAX's collectives and lax.ppermute only.
A program may use at most 32 MiB of HBM per device.

```python
import math
import jax
import jax.numpy as jnp
from jax import lax

D = 4096
H = 16
DK = 128
DV = 128
SEQS = 4
SEG = 192
LEN = 6144


def draw_tokens(key, part):
    sample_key, scale_key = jax.random.split(key, 2)
    sample = jnp.clip(jax.random.normal(sample_key, (SEQS, LEN, D)), -5.0, 5.0)
    scales = jnp.exp(jax.random.uniform(scale_key, (SEQS, LEN, 1), minval=0.0, maxval=math.log(10.0)))
    return (sample * scales).astype(jnp.bfloat16)


def draw_gap(key, part):
    order_key, slow_key, fast_key = jax.random.split(key, 3)
    ranking = jax.random.permutation(order_key, H)
    keep_count = H // 2
    slow_head = (ranking < keep_count)[:, None]
    slow_gap = jnp.exp(jax.random.uniform(slow_key, (H, DK), minval=math.log(0.2), maxval=math.log(0.8))) / LEN
    fast_gap = jnp.exp(jax.random.uniform(fast_key, (H, DK), minval=math.log(0.02), maxval=math.log(0.06)))
    return jnp.where(slow_head, slow_gap, fast_gap).astype(jnp.float32)


def draw_decay_shift(key, part):
    rate_random_key, spot_key, depth_key, closing_key = jax.random.split(key, 4)
    block_count = LEN // SEG
    low_rate, high_rate = (0.05, 0.5)
    rates = jnp.exp(jax.random.uniform(rate_random_key, (SEQS, block_count, 1, H), minval=math.log(low_rate), maxval=math.log(high_rate))) / LEN
    reference_floor = jnp.broadcast_to(rates, (SEQS, block_count, SEG, H)).reshape(SEQS, LEN, H)
    spots = jax.random.randint(spot_key, (SEQS, 2, H), 0, LEN)
    layer_depths = jax.random.uniform(depth_key, (SEQS, 2, H), minval=0.22, maxval=0.69)
    places = jnp.arange(LEN, dtype=jnp.int32)
    spike_hits = places[None, None, :, None] == spots[:, :, None, :]
    spike_events = jnp.sum(jnp.where(spike_hits, layer_depths[:, :, None, :], 0.0), axis=1)
    closing_depth = jax.random.uniform(closing_key, (SEQS, 1, H), minval=1.2, maxval=1.4)
    closing_rows = (places >= LEN - 3)[None, :, None]
    closing_events = jnp.where(closing_rows, closing_depth, 0.0)
    return (-reference_floor - spike_events - closing_events).astype(jnp.float32)


def levels(rng, dims, shards, smallest, largest):
    factor_of = 1.0
    for axis_at, shards_of in shards:
        draws = jax.random.uniform(jax.random.fold_in(jax.random.fold_in(rng, 6), axis_at), (shards_of,), jnp.float32, smallest / len(shards), largest / len(shards))
        factor_of = factor_of * jnp.repeat(jnp.exp(draws), dims[axis_at] // shards_of).reshape((-1,) + (1,) * (len(dims) - 1 - axis_at))
    return factor_of


def normal_values(stream_key, extent, scale, reach, cuts=(), kind=jnp.bfloat16):
    level = levels(stream_key, extent, cuts, -0.22, 0.18) if cuts else 1.0
    values = jax.random.normal(stream_key, extent, jnp.float32) * scale * level
    return jnp.minimum(jnp.maximum(values, -reach), reach).astype(kind)


def setup_inputs(seed: int = 0, part: int = 0) -> dict:
    streams_of = jax.random.split(jax.random.key(seed), 10)
    part_splits = jax.random.split(jax.random.fold_in(streams_of[9], part), 10)
    return {
        "tokens": draw_tokens(jax.random.fold_in(jax.random.fold_in(streams_of[9], part), 71), part),
        "new_tokens": normal_values(part_splits[1], (SEQS, D), 1.0, 6.0),
        "in_gain": jnp.clip(1.0 + 0.18 * jax.random.normal(streams_of[2], (D,), jnp.float32), 0.1, 1.9),
        "w_forget": normal_values(streams_of[3], (D, H * DK), D ** -0.5, 0.09375, ((1, 8),)),
        "w_value": normal_values(streams_of[4], (D, H * DV), (D // 64) ** -0.5, 0.75, ((1, 8),)),
        "gap": draw_gap(jax.random.fold_in(streams_of[9], 71), part),
        "decay_shift": draw_decay_shift(jax.random.fold_in(jax.random.fold_in(streams_of[9], part), 71), part),
        "query": normal_values(part_splits[7], (SEQS, H, DK), 1.0, 6.0, ((1, 8), (2, 32))),
        "out_gain": jnp.clip(1.0 + 0.18 * jax.random.normal(streams_of[8], (H, DV), jnp.float32), 0.1, 1.9),
    }


epsilon = 1e-06

def normalize(row_block, gain_row):
    widened = row_block.astype(jnp.float32)
    scaled = widened * lax.rsqrt(lax.optimization_barrier(jnp.mean(widened * widened, axis=-1, keepdims=True)) + epsilon)
    return (scaled * gain_row).astype(jnp.bfloat16)

def reference(tokens, new_tokens, in_gain, w_forget, w_value, gap, decay_shift, query, out_gain):
    block_count = LEN // SEG

    def one_prompt(inputs):
        seq_rows, decay_factor_row = inputs
        unit_norm_rows = normalize(seq_rows, in_gain)
        forget_pre = jnp.dot(unit_norm_rows, w_forget, preferred_element_type=jnp.float32).reshape(LEN, H, DK)
        values = lax.optimization_barrier(jnp.dot(unit_norm_rows, w_value, preferred_element_type=jnp.float32).astype(jnp.bfloat16))
        values = values.astype(jnp.float32).reshape(block_count, SEG, H, DV)
        key_gate = gap * jax.nn.sigmoid(-forget_pre)
        forget_logarithm = jnp.log1p(-key_gate) + decay_factor_row[:, :, None]
        blocks = forget_logarithm.reshape(block_count, SEG, H, DK)
        totals = lax.optimization_barrier(jnp.sum(blocks, axis=1))
        within = totals[:, None] - jnp.cumsum(blocks, axis=1)
        weights = lax.optimization_barrier((key_gate.reshape(block_count, SEG, H, DK) * jnp.exp(within)).astype(jnp.bfloat16))
        pieces = jnp.einsum('gthi,gthj->ghij', weights.astype(jnp.float32), values)
        later_sum = jnp.cumsum(totals[::-1], axis=0)[::-1] - totals
        return lax.optimization_barrier(jnp.sum(jnp.exp(later_sum)[..., None] * pieces, axis=0))
    full_state = lax.map(one_prompt, (tokens, decay_shift))
    cache = full_state.astype(jnp.bfloat16)
    normed_new = normalize(new_tokens, in_gain)
    new_pre = jnp.dot(normed_new, w_forget, preferred_element_type=jnp.float32).reshape(SEQS, H, DK)
    new_key = gap * jax.nn.sigmoid(-new_pre)
    new_values = lax.optimization_barrier(jnp.dot(normed_new, w_value, preferred_element_type=jnp.float32).astype(jnp.bfloat16))
    new_values = new_values.astype(jnp.float32).reshape(SEQS, H, DV)
    updated = (1.0 - new_key)[..., None] * full_state + new_key[..., None] * new_values[:, :, None, :]
    read_raw = jnp.einsum('shi,shij->shj', query.astype(jnp.float32), updated, precision=lax.Precision.HIGHEST)
    read = read_raw * lax.rsqrt(lax.optimization_barrier(jnp.mean(read_raw * read_raw, axis=-1, keepdims=True)) + epsilon) * out_gain
    return (cache, read)
```

```python
import functools

import jax
import jax.numpy as jnp
from jax import lax
from jax.experimental import pallas as pl
from jax.experimental.pallas import tpu as pltpu
from jax.sharding import PartitionSpec as P

epsilon = 1e-06

STATE_ROWS = 32
BLOCK_ROWS = 33
K_BLOCK = 512


def segment_kernel(
    seqs, heads, key_dim, steps,
    tok_ref, new_ref, gain_ref, wf_ref, wv_ref, gap_ref, shift_ref,
    buf_ref, nk_ref, nv_ref,
    accf, accv, ssq, pieces, shift_cols, total_cols,
):
    step = pl.program_id(0)
    seg = tok_ref.shape[1]
    rows = seqs * seg
    width = heads * key_dim
    pad = accf.shape[0] - rows
    groups = seqs * heads
    rank = BLOCK_ROWS
    per = STATE_ROWS // groups
    devices = key_dim // per

    tok = tok_ref[...].reshape(rows, tok_ref.shape[2])
    new = new_ref[...].astype(jnp.float32)
    new = jnp.concatenate([new, jnp.zeros((pad - seqs, new.shape[1]), jnp.float32)], axis=0)
    wide = jnp.concatenate([tok.astype(jnp.float32), new], axis=0)
    squares = wide * wide
    part = squares[:, 0:128]
    for c in range(1, squares.shape[1] // 128):
        part = part + squares[:, c * 128 : (c + 1) * 128]
    x = (wide * gain_ref[...]).astype(jnp.bfloat16)
    yf = jnp.dot(x, wf_ref[...], preferred_element_type=jnp.float32)
    yv = jnp.dot(x, wv_ref[...], preferred_element_type=jnp.float32)

    @pl.when(step == 0)
    def _():
        accf[...] = yf
        accv[...] = yv
        ssq[...] = part
        shift_rows = jnp.concatenate(
            [shift_ref[s] for s in range(seqs)]
            + [jnp.zeros((128 - groups, seg), jnp.float32)], axis=0)
        shift_rows = jnp.concatenate(
            [shift_rows, jnp.zeros((128, 256 - seg), jnp.float32)], axis=1)
        shift_cols[...] = shift_rows.T

    @pl.when(step > 0)
    def _():
        accf[...] += yf
        accv[...] += yv
        ssq[...] += part

    @pl.when(step == steps - 1)
    def _():
        model_width = steps * tok_ref.shape[2]
        gap_row = jnp.concatenate([gap_ref[h : h + 1, :] for h in range(heads)], axis=1)
        ti = lax.broadcasted_iota(jnp.int32, (seg, seg), 0)
        tj = lax.broadcasted_iota(jnp.int32, (seg, seg), 1)
        later = (tj > ti).astype(jnp.float32).astype(jnp.bfloat16)
        total_rows = []
        for s in range(seqs):
            here = slice(s * seg, (s + 1) * seg)
            scale = lax.rsqrt(
                jnp.sum(ssq[here, :], axis=1, keepdims=True) / model_width + epsilon)
            key_gate = gap_row * jax.nn.sigmoid(-(accf[here, :] * scale))
            shift = jnp.concatenate(
                [jnp.broadcast_to(shift_cols[0:seg, s * heads + h : s * heads + h + 1],
                                  (seg, key_dim)) for h in range(heads)], axis=1)
            log_forget = jnp.log1p(-key_gate) + shift
            high = log_forget.astype(jnp.bfloat16)
            low = (log_forget - high.astype(jnp.float32)).astype(jnp.bfloat16)
            within = jnp.dot(later, high, preferred_element_type=jnp.float32)
            within = within + jnp.dot(later, low, preferred_element_type=jnp.float32)
            weights = (key_gate * jnp.exp(within)).astype(jnp.bfloat16)
            values = (accv[here, :] * scale).astype(jnp.bfloat16)
            total = jnp.sum(log_forget, axis=0, keepdims=True)
            for h in range(heads):
                lanes = slice(h * key_dim, (h + 1) * key_dim)
                group = s * heads + h
                total_rows.append(total[:, lanes])
                pieces[...] = lax.dot_general(
                    weights[:, lanes], values[:, lanes], (((0,), (0,)), ((), ())),
                    preferred_element_type=jnp.float32)
                for i in range(per):
                    buf_ref[pl.ds(i * groups + group, devices, stride=rank), :] = (
                        pieces[pl.ds(i, devices, stride=per), :])
        totals = jnp.concatenate(
            total_rows + [jnp.zeros((128 - groups, key_dim), jnp.float32)], axis=0)
        total_cols[...] = totals.T
        packed = total_cols[pl.ds(0, devices, stride=per), :]
        for i in range(1, per):
            packed = packed + pltpu.roll(
                total_cols[pl.ds(i, devices, stride=per), :], i * groups, 1)
        buf_ref[pl.ds(STATE_ROWS, devices, stride=rank), :] = packed
        for extra in range(STATE_ROWS + 1, rank):
            buf_ref[pl.ds(extra, devices, stride=rank), :] = jnp.zeros_like(packed)

        last = slice(rows, rows + pad)
        scale = lax.rsqrt(
            jnp.sum(ssq[last, :], axis=1, keepdims=True) / model_width + epsilon)
        new_key = gap_row * jax.nn.sigmoid(-(accf[last, :] * scale))
        new_values = (accv[last, :] * scale).astype(jnp.bfloat16).astype(jnp.float32)
        for h in range(heads):
            lanes = slice(h * key_dim, (h + 1) * key_dim)
            nk_ref[pl.ds(h, seqs, stride=heads), :] = new_key[0:seqs, lanes]
            nv_ref[pl.ds(h, seqs, stride=heads), :] = new_values[0:seqs, lanes]


def settle_kernel(
    devices, per,
    place_ref, got_ref, nk_ref, nv_ref, query_ref,
    state_ref, part_ref,
):
    groups = nk_ref.shape[0]
    totals = got_ref[pl.ds(STATE_ROWS, devices, stride=BLOCK_ROWS), :]
    cols = jnp.concatenate(
        [totals, jnp.zeros((128 - devices, 128), jnp.float32)], axis=0).T[0:STATE_ROWS]
    later = pltpu.roll(cols, 127, 1)
    reach = 1
    while reach < devices:
        later = later + pltpu.roll(later, 128 - reach, 1)
        reach *= 2
    factor = jnp.exp(later)
    lane = lax.broadcasted_iota(jnp.int32, (groups, 128), 1)
    first = place_ref[0] * per
    query = jnp.concatenate(
        [query_ref[s].astype(jnp.float32) for s in range(query_ref.shape[0])], axis=0)
    part = jnp.zeros((groups, 128), jnp.float32)
    for i in range(per):
        base = i * groups
        state = factor[base : base + groups, 0:1] * got_ref[base : base + groups, :]
        for g in range(1, devices):
            start = g * BLOCK_ROWS + base
            state = state + factor[base : base + groups, g : g + 1] * got_ref[
                start : start + groups, :]
        state_ref[pl.ds(i, groups, stride=per), :] = state
        new_key = jnp.sum(
            jnp.where(lane == first + i, nk_ref[...], 0.0), axis=1, keepdims=True)
        updated = (1.0 - new_key) * state + new_key * nv_ref[...]
        part = part + query[:, i : i + 1] * updated
    for d in range(devices):
        part_ref[d * groups : (d + 1) * groups, :] = part


def read_kernel(devices, got_ref, gain_ref, read_ref):
    seqs, heads, val_dim = read_ref.shape
    groups = seqs * heads
    raw = got_ref[0:groups, :]
    for d in range(1, devices):
        raw = raw + got_ref[d * groups : (d + 1) * groups, :]
    gain = jnp.concatenate([gain_ref[...]] * seqs, axis=0)
    mean = jnp.sum(raw * raw, axis=1, keepdims=True) / val_dim
    out = raw * lax.rsqrt(mean + epsilon) * gain
    for s in range(seqs):
        read_ref[s] = out[s * heads : (s + 1) * heads, :]


def local(tokens, new_tokens, in_gain, w_forget, w_value, gap, decay_shift, query, out_gain):
    seqs, seg, model_width = tokens.shape
    heads, key_dim = gap.shape
    val_dim = out_gain.shape[1]
    width = heads * key_dim
    devices = lax.axis_size("sp")
    per = key_dim // devices
    groups = seqs * heads
    steps = model_width // K_BLOCK
    rows = seqs * seg + 16
    whole = pl.BlockSpec(memory_space=pltpu.VMEM)
    f32 = jnp.float32
    buf, new_key, new_values = pl.pallas_call(
        functools.partial(segment_kernel, seqs, heads, key_dim, steps),
        grid=(steps,),
        in_specs=[
            pl.BlockSpec((seqs, seg, K_BLOCK), lambda k: (0, 0, k)),
            pl.BlockSpec((seqs, K_BLOCK), lambda k: (0, k)),
            pl.BlockSpec((1, K_BLOCK), lambda k: (0, k)),
            pl.BlockSpec((K_BLOCK, width), lambda k: (k, 0)),
            pl.BlockSpec((K_BLOCK, width), lambda k: (k, 0)),
            pl.BlockSpec((heads, key_dim), lambda k: (0, 0)),
            pl.BlockSpec((seqs, heads, seg), lambda k: (0, 0, 0)),
        ],
        out_specs=[
            pl.BlockSpec((devices * BLOCK_ROWS, val_dim), lambda k: (0, 0)),
            pl.BlockSpec((groups, key_dim), lambda k: (0, 0)),
            pl.BlockSpec((groups, val_dim), lambda k: (0, 0)),
        ],
        out_shape=[
            jax.ShapeDtypeStruct((devices * BLOCK_ROWS, val_dim), f32),
            jax.ShapeDtypeStruct((groups, key_dim), f32),
            jax.ShapeDtypeStruct((groups, val_dim), f32),
        ],
        scratch_shapes=[
            pltpu.VMEM((rows, width), f32),
            pltpu.VMEM((rows, width), f32),
            pltpu.VMEM((rows, 128), f32),
            pltpu.VMEM((key_dim, val_dim), f32),
            pltpu.VMEM((256, 128), f32),
            pltpu.VMEM((128, 128), f32),
        ],
        compiler_params=pltpu.CompilerParams(
            dimension_semantics=("arbitrary",)),
        name="segment",
    )(
        tokens, new_tokens, in_gain.reshape(1, model_width), w_forget, w_value, gap,
        jnp.transpose(decay_shift, (0, 2, 1)),
    )
    got = lax.all_to_all(
        buf.reshape(devices, BLOCK_ROWS, 1, val_dim), "sp", 0, 0, tiled=True
    ).reshape(devices * BLOCK_ROWS, val_dim)
    place = lax.axis_index("sp").astype(jnp.int32).reshape(1)
    state, part = pl.pallas_call(
        functools.partial(settle_kernel, devices, per),
        in_specs=[pl.BlockSpec(memory_space=pltpu.SMEM), whole, whole, whole, whole],
        out_specs=[whole, whole],
        out_shape=[
            jax.ShapeDtypeStruct((STATE_ROWS, val_dim), f32),
            jax.ShapeDtypeStruct((devices * groups, val_dim), f32),
        ],
        compiler_params=pltpu.CompilerParams(vmem_limit_bytes=8 * 2**20),
        name="settle",
    )(place, got, new_key, new_values, query)
    everything = lax.all_to_all(
        part.reshape(devices, groups, val_dim), "sp", 0, 0, tiled=True
    ).reshape(devices * groups, val_dim)
    cache = state.astype(jnp.bfloat16).reshape(seqs, heads, per, val_dim)
    read = pl.pallas_call(
        functools.partial(read_kernel, devices),
        in_specs=[whole, whole],
        out_specs=whole,
        out_shape=jax.ShapeDtypeStruct((seqs, heads, val_dim), f32),
        compiler_params=pltpu.CompilerParams(vmem_limit_bytes=8 * 2**20),
        name="read",
    )(everything, out_gain)
    return (cache, read)


def solution(mesh):
    return jax.shard_map(
        local,
        mesh=mesh,
        in_specs=(
            P("gr", "sp", None),
            P("gr", None),
            P(),
            P(None, "tp"),
            P(None, "tp"),
            P("tp", None),
            P("gr", "sp", "tp"),
            P("gr", "tp", "sp"),
            P("tp", None),
        ),
        out_specs=(P("gr", "tp", "sp", None), P("gr", "tp", None)),
        check_vma=False,
    )
```

```python
import functools

import jax
import jax.numpy as jnp
from jax import lax
from jax.experimental import pallas as pl
from jax.experimental.pallas import tpu as pltpu
from jax.sharding import PartitionSpec as P

epsilon = 1e-06

STATE_ROWS = 32
BLOCK_ROWS = 33
CHUNKS = (512, 512, 1024, 1024, 1024)
VMEM_MIB = 48


def segment_kernel(
    seqs, heads, key_dim, chunks,
    tok_hbm, new_hbm, gain_hbm, wf_hbm, wv_hbm, gap_hbm, shift_hbm,
    buf_ref, nk_ref, nv_ref,
    tok_ref, wf_ref, wv_ref, new_ref, gain_ref, gap_ref, shift_ref, accf, accv, ssq, pieces, shift_cols, total_cols, sems,
):
    seg = tok_ref.shape[1]
    model_width = tok_ref.shape[2]
    rows = seqs * seg
    pad = accf.shape[0] - rows
    groups = seqs * heads
    rank = BLOCK_ROWS
    per = STATE_ROWS // groups
    devices = key_dim // per

    small = [
        pltpu.make_async_copy(source, target, sems.at[3, n])
        for n, (source, target) in enumerate(
            ((new_hbm, new_ref), (gain_hbm, gain_ref), (gap_hbm, gap_ref),
             (shift_hbm, shift_ref)))
    ]
    copies = []
    start = 0
    for n, size in enumerate(chunks):
        cols = slice(start, start + size)
        trio = [
            pltpu.make_async_copy(wf_hbm.at[cols, :], wf_ref.at[cols, :], sems.at[0, n]),
            pltpu.make_async_copy(wv_hbm.at[cols, :], wv_ref.at[cols, :], sems.at[1, n]),
            pltpu.make_async_copy(tok_hbm.at[:, :, cols], tok_ref.at[:, :, cols], sems.at[2, n]),
        ]
        for copy in trio:
            copy.start()
        if n == 0:
            for copy in small:
                copy.start()
        copies.append((cols, trio))
        start += size
    for copy in small:
        copy.wait()
    shift_rows = jnp.concatenate(
        [shift_ref[s] for s in range(seqs)]
        + [jnp.zeros((128 - groups, seg), jnp.float32)], axis=0)
    shift_rows = jnp.concatenate(
        [shift_rows, jnp.zeros((128, 256 - seg), jnp.float32)], axis=1)
    shift_cols[...] = shift_rows.T

    for n, (cols, trio) in enumerate(copies):
        for copy in trio:
            copy.wait()
        wide = tok_ref[:, :, cols].reshape(rows, chunks[n]).astype(jnp.float32)
        new = new_ref[:, cols].astype(jnp.float32)
        new = jnp.concatenate([new, jnp.zeros((pad - seqs, chunks[n]), jnp.float32)], axis=0)
        wide = jnp.concatenate([wide, new], axis=0)
        squares = wide * wide
        part = squares[:, 0:128]
        for c in range(1, chunks[n] // 128):
            part = part + squares[:, c * 128 : (c + 1) * 128]
        x = (wide * gain_ref[:, cols]).astype(jnp.bfloat16)
        yf = jnp.dot(x, wf_ref[cols, :], preferred_element_type=jnp.float32)
        yv = jnp.dot(x, wv_ref[cols, :], preferred_element_type=jnp.float32)
        if n == 0:
            accf[...] = yf
            accv[...] = yv
            ssq[...] = part
        else:
            accf[...] += yf
            accv[...] += yv
            ssq[...] += part

    gap_row = jnp.concatenate([gap_ref[h : h + 1, :] for h in range(heads)], axis=1)
    ti = lax.broadcasted_iota(jnp.int32, (seg, seg), 0)
    tj = lax.broadcasted_iota(jnp.int32, (seg, seg), 1)
    later = (tj > ti).astype(jnp.float32).astype(jnp.bfloat16)
    total_rows = []
    for s in range(seqs):
        here = slice(s * seg, (s + 1) * seg)
        scale = lax.rsqrt(
            jnp.sum(ssq[here, :], axis=1, keepdims=True) / model_width + epsilon)
        key_gate = gap_row * jax.nn.sigmoid(-(accf[here, :] * scale))
        shift = jnp.concatenate(
            [jnp.broadcast_to(shift_cols[0:seg, s * heads + h : s * heads + h + 1],
                              (seg, key_dim)) for h in range(heads)], axis=1)
        log_forget = jnp.log1p(-key_gate) + shift
        high = log_forget.astype(jnp.bfloat16)
        low = (log_forget - high.astype(jnp.float32)).astype(jnp.bfloat16)
        within = jnp.dot(later, high, preferred_element_type=jnp.float32)
        within = within + jnp.dot(later, low, preferred_element_type=jnp.float32)
        weights = (key_gate * jnp.exp(within)).astype(jnp.bfloat16)
        values = (accv[here, :] * scale).astype(jnp.bfloat16)
        total = jnp.sum(log_forget, axis=0, keepdims=True)
        for h in range(heads):
            lanes = slice(h * key_dim, (h + 1) * key_dim)
            group = s * heads + h
            total_rows.append(total[:, lanes])
            pieces[...] = lax.dot_general(
                weights[:, lanes], values[:, lanes], (((0,), (0,)), ((), ())),
                preferred_element_type=jnp.float32)
            for i in range(per):
                buf_ref[pl.ds(i * groups + group, devices, stride=rank), :] = (
                    pieces[pl.ds(i, devices, stride=per), :])
    totals = jnp.concatenate(
        total_rows + [jnp.zeros((128 - groups, key_dim), jnp.float32)], axis=0)
    total_cols[...] = totals.T
    packed = total_cols[pl.ds(0, devices, stride=per), :]
    for i in range(1, per):
        packed = packed + pltpu.roll(
            total_cols[pl.ds(i, devices, stride=per), :], i * groups, 1)
    buf_ref[pl.ds(STATE_ROWS, devices, stride=rank), :] = packed
    for extra in range(STATE_ROWS + 1, rank):
        buf_ref[pl.ds(extra, devices, stride=rank), :] = jnp.zeros_like(packed)

    last = slice(rows, rows + pad)
    scale = lax.rsqrt(
        jnp.sum(ssq[last, :], axis=1, keepdims=True) / model_width + epsilon)
    new_key = gap_row * jax.nn.sigmoid(-(accf[last, :] * scale))
    new_values = (accv[last, :] * scale).astype(jnp.bfloat16).astype(jnp.float32)
    for h in range(heads):
        lanes = slice(h * key_dim, (h + 1) * key_dim)
        nk_ref[pl.ds(h, seqs, stride=heads), :] = new_key[0:seqs, lanes]
        nv_ref[pl.ds(h, seqs, stride=heads), :] = new_values[0:seqs, lanes]


def settle_kernel(
    devices, per,
    place_ref, got_ref, nk_ref, nv_ref, query_ref,
    cache_ref, part_ref, state_ref,
):
    groups = nk_ref.shape[0]
    totals = got_ref[pl.ds(STATE_ROWS, devices, stride=BLOCK_ROWS), :]
    cols = jnp.concatenate(
        [totals, jnp.zeros((128 - devices, 128), jnp.float32)], axis=0).T[0:STATE_ROWS]
    later = pltpu.roll(cols, 127, 1)
    reach = 1
    while reach < devices:
        later = later + pltpu.roll(later, 128 - reach, 1)
        reach *= 2
    factor = jnp.exp(later)
    lane = lax.broadcasted_iota(jnp.int32, (groups, 128), 1)
    first = place_ref[0] * per
    query = jnp.concatenate(
        [query_ref[s].astype(jnp.float32) for s in range(query_ref.shape[0])], axis=0)
    part = jnp.zeros((groups, 128), jnp.float32)
    for i in range(per):
        base = i * groups
        state = factor[base : base + groups, 0:1] * got_ref[base : base + groups, :]
        for g in range(1, devices):
            start = g * BLOCK_ROWS + base
            state = state + factor[base : base + groups, g : g + 1] * got_ref[
                start : start + groups, :]
        state_ref[pl.ds(i, groups, stride=per), :] = state
        new_key = jnp.sum(
            jnp.where(lane == first + i, nk_ref[...], 0.0), axis=1, keepdims=True)
        updated = (1.0 - new_key) * state + new_key * nv_ref[...]
        part = part + query[:, i : i + 1] * updated
    cache_ref[...] = state_ref[...].astype(jnp.bfloat16)
    for d in range(devices):
        part_ref[d * groups : (d + 1) * groups, :] = part


def read_kernel(devices, got_ref, gain_ref, read_ref):
    seqs, heads, val_dim = read_ref.shape
    groups = seqs * heads
    raw = got_ref[0:groups, :]
    for d in range(1, devices):
        raw = raw + got_ref[d * groups : (d + 1) * groups, :]
    gain = jnp.concatenate([gain_ref[...]] * seqs, axis=0)
    mean = jnp.sum(raw * raw, axis=1, keepdims=True) / val_dim
    out = raw * lax.rsqrt(mean + epsilon) * gain
    for s in range(seqs):
        read_ref[s] = out[s * heads : (s + 1) * heads, :]


def segments(tokens, new_tokens, gain_row, w_forget, w_value, gap, shift_rows):
    seqs, seg, model_width = tokens.shape
    heads, key_dim = gap.shape
    width = w_forget.shape[1]
    val_dim = width // heads
    groups = seqs * heads
    devices = key_dim * groups // STATE_ROWS
    rows = seqs * seg + 16
    f32 = jnp.float32
    whole = pl.BlockSpec(memory_space=pltpu.VMEM)
    hbm = pl.BlockSpec(memory_space=pltpu.HBM)
    return pl.pallas_call(
        functools.partial(segment_kernel, seqs, heads, key_dim, CHUNKS),
        in_specs=[hbm] * 7,
        out_specs=[whole, whole, whole],
        out_shape=[
            jax.ShapeDtypeStruct((devices * BLOCK_ROWS, val_dim), f32),
            jax.ShapeDtypeStruct((groups, key_dim), f32),
            jax.ShapeDtypeStruct((groups, val_dim), f32),
        ],
        scratch_shapes=[
            pltpu.VMEM((seqs, seg, model_width), jnp.bfloat16),
            pltpu.VMEM((model_width, width), jnp.bfloat16),
            pltpu.VMEM((model_width, width), jnp.bfloat16),
            pltpu.VMEM((seqs, model_width), jnp.bfloat16),
            pltpu.VMEM((1, model_width), f32),
            pltpu.VMEM((heads, key_dim), f32),
            pltpu.VMEM((seqs, heads, seg), f32),
            pltpu.VMEM((rows, width), f32),
            pltpu.VMEM((rows, width), f32),
            pltpu.VMEM((rows, 128), f32),
            pltpu.VMEM((key_dim, val_dim), f32),
            pltpu.VMEM((256, 128), f32),
            pltpu.VMEM((128, 128), f32),
            pltpu.SemaphoreType.DMA((4, max(4, len(CHUNKS)))),
        ],
        compiler_params=pltpu.CompilerParams(vmem_limit_bytes=VMEM_MIB * 2**20),
        name="segment",
    )(
        *(pltpu.with_memory_space_constraint(x, pltpu.HBM) for x in (
            tokens, new_tokens, gain_row, w_forget, w_value, gap, shift_rows))
    )


def local(tokens, new_tokens, in_gain, w_forget, w_value, gap, decay_shift, query, out_gain):
    seqs, seg, model_width = tokens.shape
    heads, key_dim = gap.shape
    val_dim = out_gain.shape[1]
    devices = lax.axis_size("sp")
    per = key_dim // devices
    groups = seqs * heads
    whole = pl.BlockSpec(memory_space=pltpu.VMEM)
    f32 = jnp.float32
    buf, new_key, new_values = segments(
        tokens, new_tokens, in_gain.reshape(1, model_width), w_forget, w_value, gap,
        jnp.transpose(decay_shift, (0, 2, 1)))
    got = lax.all_to_all(
        buf.reshape(devices, BLOCK_ROWS, 1, val_dim), "sp", 0, 0, tiled=True
    ).reshape(devices * BLOCK_ROWS, val_dim)
    place = lax.axis_index("sp").astype(jnp.int32).reshape(1)
    cache, part = pl.pallas_call(
        functools.partial(settle_kernel, devices, per),
        in_specs=[pl.BlockSpec(memory_space=pltpu.SMEM), whole, whole, whole, whole],
        out_specs=[whole, whole],
        out_shape=[
            jax.ShapeDtypeStruct((STATE_ROWS, val_dim), jnp.bfloat16),
            jax.ShapeDtypeStruct((devices * groups, val_dim), f32),
        ],
        scratch_shapes=[pltpu.VMEM((STATE_ROWS, val_dim), f32)],
        compiler_params=pltpu.CompilerParams(vmem_limit_bytes=8 * 2**20),
        name="settle",
    )(place, got, new_key, new_values, query)
    everything = lax.all_to_all(
        part.reshape(devices, groups, val_dim), "sp", 0, 0, tiled=True
    ).reshape(devices * groups, val_dim)
    read = pl.pallas_call(
        functools.partial(read_kernel, devices),
        in_specs=[whole, whole],
        out_specs=whole,
        out_shape=jax.ShapeDtypeStruct((seqs, heads, val_dim), f32),
        compiler_params=pltpu.CompilerParams(vmem_limit_bytes=8 * 2**20),
        name="read",
    )(everything, out_gain)
    return (cache.reshape(seqs, heads, per, val_dim), read)


def solution(mesh):
    return jax.shard_map(
        local,
        mesh=mesh,
        in_specs=(
            P("gr", "sp", None),
            P("gr", None),
            P(),
            P(None, "tp"),
            P(None, "tp"),
            P("tp", None),
            P("gr", "sp", "tp"),
            P("gr", "tp", "sp"),
            P("tp", None),
        ),
        out_specs=(P("gr", "tp", "sp", None), P("gr", "tp", None)),
        check_vma=False,
    )
```

```python
import functools

import jax
import jax.numpy as jnp
from jax import lax
from jax.experimental import pallas as pl
from jax.experimental.pallas import tpu as pltpu
from jax.sharding import PartitionSpec as P

epsilon = 1e-06

STATE_ROWS = 32
BLOCK_ROWS = 33
CHUNKS = (512,) * 8
VMEM_MIB = 48


def segment_kernel(
    seqs, heads, key_dim, chunks,
    tok_hbm, new_hbm, gain_hbm, wf_hbm, wv_hbm, gap_hbm, shift_hbm,
    buf_ref, nk_ref, nv_ref,
    tok_ref, wf_ref, wv_ref, new_ref, gain_ref, gap_ref, shift_ref, accf, accv, ssq, pieces, shift_cols, total_cols, sems,
):
    seg = tok_ref.shape[1]
    model_width = tok_ref.shape[2]
    rows = seqs * seg
    pad = accf.shape[0] - rows
    groups = seqs * heads
    rank = BLOCK_ROWS
    per = STATE_ROWS // groups
    devices = key_dim // per

    small = [
        pltpu.make_async_copy(source, target, sems.at[3, n])
        for n, (source, target) in enumerate(
            ((new_hbm, new_ref), (gain_hbm, gain_ref), (gap_hbm, gap_ref),
             (shift_hbm, shift_ref)))
    ]
    copies = []
    start = 0
    for n, size in enumerate(chunks):
        cols = slice(start, start + size)
        trio = [
            pltpu.make_async_copy(wf_hbm.at[cols, :], wf_ref.at[cols, :], sems.at[0, n]),
            pltpu.make_async_copy(wv_hbm.at[cols, :], wv_ref.at[cols, :], sems.at[1, n]),
            pltpu.make_async_copy(tok_hbm.at[:, :, cols], tok_ref.at[:, :, cols], sems.at[2, n]),
        ]
        for copy in trio:
            copy.start()
        if n == 0:
            for copy in small:
                copy.start()
        copies.append((cols, trio))
        start += size
    for copy in small:
        copy.wait()
    shift_rows = jnp.concatenate(
        [shift_ref[s] for s in range(seqs)]
        + [jnp.zeros((128 - groups, seg), jnp.float32)], axis=0)
    shift_rows = jnp.concatenate(
        [shift_rows, jnp.zeros((128, 256 - seg), jnp.float32)], axis=1)
    shift_cols[...] = shift_rows.T

    for n, (cols, trio) in enumerate(copies):
        for copy in trio:
            copy.wait()
        wide = tok_ref[:, :, cols].reshape(rows, chunks[n]).astype(jnp.float32)
        new = new_ref[:, cols].astype(jnp.float32)
        new = jnp.concatenate([new, jnp.zeros((pad - seqs, chunks[n]), jnp.float32)], axis=0)
        wide = jnp.concatenate([wide, new], axis=0)
        squares = wide * wide
        part = squares[:, 0:128]
        for c in range(1, chunks[n] // 128):
            part = part + squares[:, c * 128 : (c + 1) * 128]
        x = (wide * gain_ref[:, cols]).astype(jnp.bfloat16)
        yf = jnp.dot(x, wf_ref[cols, :], preferred_element_type=jnp.float32)
        yv = jnp.dot(x, wv_ref[cols, :], preferred_element_type=jnp.float32)
        if n == 0:
            accf[...] = yf
            accv[...] = yv
            ssq[...] = part
        else:
            accf[...] += yf
            accv[...] += yv
            ssq[...] += part

    gap_row = jnp.concatenate([gap_ref[h : h + 1, :] for h in range(heads)], axis=1)
    ti = lax.broadcasted_iota(jnp.int32, (seg, seg), 0)
    tj = lax.broadcasted_iota(jnp.int32, (seg, seg), 1)
    later = (tj > ti).astype(jnp.float32).astype(jnp.bfloat16)
    total_rows = []
    for s in range(seqs):
        here = slice(s * seg, (s + 1) * seg)
        scale = lax.rsqrt(
            jnp.sum(ssq[here, :], axis=1, keepdims=True) / model_width + epsilon)
        key_gate = gap_row * jax.nn.sigmoid(-(accf[here, :] * scale))
        shift = jnp.concatenate(
            [jnp.broadcast_to(shift_cols[0:seg, s * heads + h : s * heads + h + 1],
                              (seg, key_dim)) for h in range(heads)], axis=1)
        log_forget = jnp.log1p(-key_gate) + shift
        high = log_forget.astype(jnp.bfloat16)
        low = (log_forget - high.astype(jnp.float32)).astype(jnp.bfloat16)
        within = jnp.dot(later, high, preferred_element_type=jnp.float32)
        within = within + jnp.dot(later, low, preferred_element_type=jnp.float32)
        weights = (key_gate * jnp.exp(within)).astype(jnp.bfloat16)
        values = (accv[here, :] * scale).astype(jnp.bfloat16)
        total = jnp.sum(log_forget, axis=0, keepdims=True)
        for h in range(heads):
            lanes = slice(h * key_dim, (h + 1) * key_dim)
            group = s * heads + h
            total_rows.append(total[:, lanes])
            pieces[...] = lax.dot_general(
                weights[:, lanes], values[:, lanes], (((0,), (0,)), ((), ())),
                preferred_element_type=jnp.float32)
            for i in range(per):
                buf_ref[pl.ds(i * groups + group, devices, stride=rank), :] = (
                    pieces[pl.ds(i, devices, stride=per), :])
    totals = jnp.concatenate(
        total_rows + [jnp.zeros((128 - groups, key_dim), jnp.float32)], axis=0)
    total_cols[...] = totals.T
    packed = total_cols[pl.ds(0, devices, stride=per), :]
    for i in range(1, per):
        packed = packed + pltpu.roll(
            total_cols[pl.ds(i, devices, stride=per), :], i * groups, 1)
    buf_ref[pl.ds(STATE_ROWS, devices, stride=rank), :] = packed
    for extra in range(STATE_ROWS + 1, rank):
        buf_ref[pl.ds(extra, devices, stride=rank), :] = jnp.zeros_like(packed)

    last = slice(rows, rows + pad)
    scale = lax.rsqrt(
        jnp.sum(ssq[last, :], axis=1, keepdims=True) / model_width + epsilon)
    new_key = gap_row * jax.nn.sigmoid(-(accf[last, :] * scale))
    new_values = (accv[last, :] * scale).astype(jnp.bfloat16).astype(jnp.float32)
    for h in range(heads):
        lanes = slice(h * key_dim, (h + 1) * key_dim)
        nk_ref[pl.ds(h, seqs, stride=heads), :] = new_key[0:seqs, lanes]
        nv_ref[pl.ds(h, seqs, stride=heads), :] = new_values[0:seqs, lanes]


def settle_kernel(
    devices, per,
    got_ref, nk_ref, nv_ref, query_ref,
    cache_ref, part_ref, state_ref,
):
    groups = nk_ref.shape[0]
    totals = got_ref[pl.ds(STATE_ROWS, devices, stride=BLOCK_ROWS), :]
    cols = jnp.concatenate(
        [totals, jnp.zeros((128 - devices, 128), jnp.float32)], axis=0).T[0:STATE_ROWS]
    later = pltpu.roll(cols, 127, 1)
    reach = 1
    while reach < devices:
        later = later + pltpu.roll(later, 128 - reach, 1)
        reach *= 2
    factor = jnp.exp(later)
    lane = lax.broadcasted_iota(jnp.int32, (groups, 128), 1)
    first = lax.axis_index("sp") * per
    query = jnp.concatenate(
        [query_ref[s].astype(jnp.float32) for s in range(query_ref.shape[0])], axis=0)
    part = jnp.zeros((groups, 128), jnp.float32)
    for i in range(per):
        base = i * groups
        state = factor[base : base + groups, 0:1] * got_ref[base : base + groups, :]
        for g in range(1, devices):
            start = g * BLOCK_ROWS + base
            state = state + factor[base : base + groups, g : g + 1] * got_ref[
                start : start + groups, :]
        state_ref[pl.ds(i, groups, stride=per), :] = state
        new_key = jnp.sum(
            jnp.where(lane == first + i, nk_ref[...], 0.0), axis=1, keepdims=True)
        updated = (1.0 - new_key) * state + new_key * nv_ref[...]
        part = part + query[:, i : i + 1] * updated
    cache_ref[...] = state_ref[...].astype(jnp.bfloat16)
    for d in range(devices):
        part_ref[d * groups : (d + 1) * groups, :] = part


def read_kernel(devices, got_ref, gain_ref, state_ref, read_ref, cache_ref):
    seqs, heads, val_dim = read_ref.shape
    cache_ref[...] = state_ref[...]
    groups = seqs * heads
    raw = got_ref[0:groups, :]
    for d in range(1, devices):
        raw = raw + got_ref[d * groups : (d + 1) * groups, :]
    gain = jnp.concatenate([gain_ref[...]] * seqs, axis=0)
    mean = jnp.sum(raw * raw, axis=1, keepdims=True) / val_dim
    out = raw * lax.rsqrt(mean + epsilon) * gain
    for s in range(seqs):
        read_ref[s] = out[s * heads : (s + 1) * heads, :]


def segments(tokens, new_tokens, gain_row, w_forget, w_value, gap, shift_rows):
    seqs, seg, model_width = tokens.shape
    heads, key_dim = gap.shape
    width = w_forget.shape[1]
    val_dim = width // heads
    groups = seqs * heads
    devices = key_dim * groups // STATE_ROWS
    rows = seqs * seg + 16
    f32 = jnp.float32
    whole = pl.BlockSpec(memory_space=pltpu.VMEM)
    hbm = pl.BlockSpec(memory_space=pltpu.HBM)
    return pl.pallas_call(
        functools.partial(segment_kernel, seqs, heads, key_dim, CHUNKS),
        in_specs=[hbm] * 7,
        out_specs=[whole, whole, whole],
        out_shape=[
            jax.ShapeDtypeStruct((devices * BLOCK_ROWS, val_dim), f32),
            jax.ShapeDtypeStruct((groups, key_dim), f32),
            jax.ShapeDtypeStruct((groups, val_dim), f32),
        ],
        scratch_shapes=[
            pltpu.VMEM((seqs, seg, model_width), jnp.bfloat16),
            pltpu.VMEM((model_width, width), jnp.bfloat16),
            pltpu.VMEM((model_width, width), jnp.bfloat16),
            pltpu.VMEM((seqs, model_width), jnp.bfloat16),
            pltpu.VMEM((1, model_width), f32),
            pltpu.VMEM((heads, key_dim), f32),
            pltpu.VMEM((seqs, heads, seg), f32),
            pltpu.VMEM((rows, width), f32),
            pltpu.VMEM((rows, width), f32),
            pltpu.VMEM((rows, 128), f32),
            pltpu.VMEM((key_dim, val_dim), f32),
            pltpu.VMEM((256, 128), f32),
            pltpu.VMEM((128, 128), f32),
            pltpu.SemaphoreType.DMA((4, max(4, len(CHUNKS)))),
        ],
        compiler_params=pltpu.CompilerParams(vmem_limit_bytes=VMEM_MIB * 2**20),
        name="segment",
    )(
        *(pltpu.with_memory_space_constraint(x, pltpu.HBM) for x in (
            tokens, new_tokens, gain_row, w_forget, w_value, gap, shift_rows))
    )


def local(tokens, new_tokens, in_gain, w_forget, w_value, gap, decay_shift, query, out_gain):
    seqs, seg, model_width = tokens.shape
    heads, key_dim = gap.shape
    val_dim = out_gain.shape[1]
    devices = lax.axis_size("sp")
    per = key_dim // devices
    groups = seqs * heads
    whole = pl.BlockSpec(memory_space=pltpu.VMEM)
    f32 = jnp.float32
    buf, new_key, new_values = segments(
        tokens, new_tokens, in_gain.reshape(1, model_width), w_forget, w_value, gap,
        jnp.transpose(decay_shift, (0, 2, 1)))
    got = lax.all_to_all(
        buf.reshape(devices, BLOCK_ROWS, 1, val_dim), "sp", 0, 0, tiled=True
    ).reshape(devices * BLOCK_ROWS, val_dim)
    state, part = pl.pallas_call(
        functools.partial(settle_kernel, devices, per),
        in_specs=[whole, whole, whole, whole],
        out_specs=[whole, whole],
        out_shape=[
            jax.ShapeDtypeStruct((STATE_ROWS, val_dim), jnp.bfloat16),
            jax.ShapeDtypeStruct((devices * groups, val_dim), f32),
        ],
        scratch_shapes=[pltpu.VMEM((STATE_ROWS, val_dim), f32)],
        compiler_params=pltpu.CompilerParams(vmem_limit_bytes=8 * 2**20),
        name="settle",
    )(got, new_key, new_values, query)
    everything = lax.all_to_all(
        part.reshape(devices, groups, val_dim), "sp", 0, 0, tiled=True
    ).reshape(devices * groups, val_dim)
    read, cache = pl.pallas_call(
        functools.partial(read_kernel, devices),
        in_specs=[whole, whole, whole],
        out_specs=[whole, whole],
        out_shape=[
            jax.ShapeDtypeStruct((seqs, heads, val_dim), f32),
            jax.ShapeDtypeStruct((STATE_ROWS, val_dim), jnp.bfloat16),
        ],
        compiler_params=pltpu.CompilerParams(vmem_limit_bytes=8 * 2**20),
        name="read",
    )(everything, out_gain, state)
    return (cache.reshape(seqs, heads, per, val_dim), read)


def solution(mesh):
    return jax.shard_map(
        local,
        mesh=mesh,
        in_specs=(
            P("gr", "sp", None),
            P("gr", None),
            P(),
            P(None, "tp"),
            P(None, "tp"),
            P("tp", None),
            P("gr", "sp", "tp"),
            P("gr", "tp", "sp"),
            P("tp", None),
        ),
        out_specs=(P("gr", "tp", "sp", None), P("gr", "tp", None)),
        check_vma=False,
    )
```

```python
import functools

import jax
import jax.numpy as jnp
from jax import lax
from jax.experimental import pallas as pl
from jax.experimental.pallas import tpu as pltpu
from jax.sharding import PartitionSpec as P

epsilon = 1e-06

STATE_ROWS = 32
BLOCK_ROWS = 33
CHUNKS = (512,) * 8
VMEM_MIB = 48


def segment_kernel(
    seqs, heads, key_dim, chunks,
    tok_hbm, new_hbm, gain_hbm, wf_hbm, wv_hbm, gap_hbm, shift_hbm,
    buf_ref, nk_ref, nv_ref,
    tok_ref, wf_ref, wv_ref, new_ref, gain_ref, gap_ref, shift_ref, accf, accv, ssq, pieces, shift_cols, shift_wide, total_cols, sems,
):
    seg = tok_ref.shape[1]
    model_width = tok_ref.shape[2]
    rows = seqs * seg
    pad = accf.shape[0] - rows
    groups = seqs * heads
    rank = BLOCK_ROWS
    per = STATE_ROWS // groups
    devices = key_dim // per

    small = [
        pltpu.make_async_copy(source, target, sems.at[3, n])
        for n, (source, target) in enumerate(
            ((new_hbm, new_ref), (gain_hbm, gain_ref), (gap_hbm, gap_ref),
             (shift_hbm, shift_ref)))
    ]
    copies = []
    start = 0
    for n, size in enumerate(chunks):
        cols = slice(start, start + size)
        trio = [
            pltpu.make_async_copy(wf_hbm.at[cols, :], wf_ref.at[cols, :], sems.at[0, n]),
            pltpu.make_async_copy(wv_hbm.at[cols, :], wv_ref.at[cols, :], sems.at[1, n]),
            pltpu.make_async_copy(tok_hbm.at[:, :, cols], tok_ref.at[:, :, cols], sems.at[2, n]),
        ]
        for copy in trio:
            copy.start()
        if n == 0:
            for copy in small:
                copy.start()
        copies.append((cols, trio))
        start += size
    for copy in small:
        copy.wait()
    shift_rows = jnp.concatenate(
        [shift_ref[s] for s in range(seqs)]
        + [jnp.zeros((128 - groups, seg), jnp.float32)], axis=0)
    shift_rows = jnp.concatenate(
        [shift_rows, jnp.zeros((128, 256 - seg), jnp.float32)], axis=1)
    shift_cols[...] = shift_rows.T

    widened = [[] for _ in chunks]
    for s in range(seqs):
        widened[min(s + 2, len(chunks) - 1)].append(s)
    for n, (cols, trio) in enumerate(copies):
        for copy in trio:
            copy.wait()
        wide = tok_ref[:, :, cols].reshape(rows, chunks[n]).astype(jnp.float32)
        new = new_ref[:, cols].astype(jnp.float32)
        new = jnp.concatenate([new, jnp.zeros((pad - seqs, chunks[n]), jnp.float32)], axis=0)
        wide = jnp.concatenate([wide, new], axis=0)
        squares = wide * wide
        part = squares[:, 0:128]
        for c in range(1, chunks[n] // 128):
            part = part + squares[:, c * 128 : (c + 1) * 128]
        x = (wide * gain_ref[:, cols]).astype(jnp.bfloat16)
        yf = jnp.dot(x, wf_ref[cols, :], preferred_element_type=jnp.float32)
        yv = jnp.dot(x, wv_ref[cols, :], preferred_element_type=jnp.float32)
        if n == 0:
            accf[...] = yf
            accv[...] = yv
            ssq[...] = part
        else:
            accf[...] += yf
            accv[...] += yv
            ssq[...] += part
        for s in widened[n]:
            for h in range(heads):
                group = s * heads + h
                shift_wide[s * seg : (s + 1) * seg, h * key_dim : (h + 1) * key_dim] = (
                    jnp.broadcast_to(shift_cols[0:seg, group : group + 1], (seg, key_dim)))

    gap_row = jnp.concatenate([gap_ref[h : h + 1, :] for h in range(heads)], axis=1)
    ti = lax.broadcasted_iota(jnp.int32, (seg, seg), 0)
    tj = lax.broadcasted_iota(jnp.int32, (seg, seg), 1)
    later = (tj > ti).astype(jnp.float32).astype(jnp.bfloat16)
    total_rows = []
    gated = []
    for s in range(seqs):
        here = slice(s * seg, (s + 1) * seg)
        scale = lax.rsqrt(
            jnp.sum(ssq[here, :], axis=1, keepdims=True) / model_width + epsilon)
        key_gate = gap_row * jax.nn.sigmoid(-(accf[here, :] * scale))
        log_forget = jnp.log1p(-key_gate) + shift_wide[here, :]
        high = log_forget.astype(jnp.bfloat16)
        low = (log_forget - high.astype(jnp.float32)).astype(jnp.bfloat16)
        within = jnp.dot(later, high, preferred_element_type=jnp.float32)
        within = within + jnp.dot(later, low, preferred_element_type=jnp.float32)
        weights = (key_gate * jnp.exp(within)).astype(jnp.bfloat16)
        values = (accv[here, :] * scale).astype(jnp.bfloat16)
        total = jnp.sum(log_forget, axis=0, keepdims=True)
        for h in range(heads):
            lanes = slice(h * key_dim, (h + 1) * key_dim)
            group = s * heads + h
            total_rows.append(total[:, lanes])
            gated.append((weights[:, lanes], values[:, lanes]))
    for group in range(groups):
        pieces[group] = lax.dot_general(
            *gated[group], (((0,), (0,)), ((), ())), preferred_element_type=jnp.float32)
    for group in range(groups):
        for i in range(per):
            buf_ref[pl.ds(i * groups + group, devices, stride=rank), :] = (
                pieces[group, pl.ds(i, devices, stride=per), :])
    totals = jnp.concatenate(
        total_rows + [jnp.zeros((128 - groups, key_dim), jnp.float32)], axis=0)
    total_cols[...] = totals.T
    packed = total_cols[pl.ds(0, devices, stride=per), :]
    for i in range(1, per):
        packed = packed + pltpu.roll(
            total_cols[pl.ds(i, devices, stride=per), :], i * groups, 1)
    buf_ref[pl.ds(STATE_ROWS, devices, stride=rank), :] = packed
    for extra in range(STATE_ROWS + 1, rank):
        buf_ref[pl.ds(extra, devices, stride=rank), :] = jnp.zeros_like(packed)

    last = slice(rows, rows + pad)
    scale = lax.rsqrt(
        jnp.sum(ssq[last, :], axis=1, keepdims=True) / model_width + epsilon)
    new_key = gap_row * jax.nn.sigmoid(-(accf[last, :] * scale))
    new_values = (accv[last, :] * scale).astype(jnp.bfloat16).astype(jnp.float32)
    for h in range(heads):
        lanes = slice(h * key_dim, (h + 1) * key_dim)
        nk_ref[pl.ds(h, seqs, stride=heads), :] = new_key[0:seqs, lanes]
        nv_ref[pl.ds(h, seqs, stride=heads), :] = new_values[0:seqs, lanes]


def settle_kernel(
    devices, per,
    got_ref, nk_ref, nv_ref, query_ref,
    cache_ref, part_ref, state_ref,
):
    groups = nk_ref.shape[0]
    totals = got_ref[pl.ds(STATE_ROWS, devices, stride=BLOCK_ROWS), :]
    cols = jnp.concatenate(
        [totals, jnp.zeros((128 - devices, 128), jnp.float32)], axis=0).T[0:STATE_ROWS]
    later = pltpu.roll(cols, 127, 1)
    reach = 1
    while reach < devices:
        later = later + pltpu.roll(later, 128 - reach, 1)
        reach *= 2
    factor = jnp.exp(later)
    lane = lax.broadcasted_iota(jnp.int32, (groups, 128), 1)
    first = lax.axis_index("sp") * per
    query = jnp.concatenate(
        [query_ref[s].astype(jnp.float32) for s in range(query_ref.shape[0])], axis=0)
    part = jnp.zeros((groups, 128), jnp.float32)
    for i in range(per):
        base = i * groups
        state = factor[base : base + groups, 0:1] * got_ref[base : base + groups, :]
        for g in range(1, devices):
            start = g * BLOCK_ROWS + base
            state = state + factor[base : base + groups, g : g + 1] * got_ref[
                start : start + groups, :]
        state_ref[pl.ds(i, groups, stride=per), :] = state
        new_key = jnp.sum(
            jnp.where(lane == first + i, nk_ref[...], 0.0), axis=1, keepdims=True)
        updated = (1.0 - new_key) * state + new_key * nv_ref[...]
        part = part + query[:, i : i + 1] * updated
    cache_ref[...] = state_ref[...].astype(jnp.bfloat16)
    for d in range(devices):
        part_ref[d * groups : (d + 1) * groups, :] = part


def read_kernel(devices, got_ref, gain_ref, state_ref, read_ref, cache_ref):
    seqs, heads, val_dim = read_ref.shape
    cache_ref[...] = state_ref[...]
    groups = seqs * heads
    raw = got_ref[0:groups, :]
    for d in range(1, devices):
        raw = raw + got_ref[d * groups : (d + 1) * groups, :]
    gain = jnp.concatenate([gain_ref[...]] * seqs, axis=0)
    mean = jnp.sum(raw * raw, axis=1, keepdims=True) / val_dim
    out = raw * lax.rsqrt(mean + epsilon) * gain
    for s in range(seqs):
        read_ref[s] = out[s * heads : (s + 1) * heads, :]


def segments(tokens, new_tokens, gain_row, w_forget, w_value, gap, shift_rows):
    seqs, seg, model_width = tokens.shape
    heads, key_dim = gap.shape
    width = w_forget.shape[1]
    val_dim = width // heads
    groups = seqs * heads
    devices = key_dim * groups // STATE_ROWS
    rows = seqs * seg + 16
    f32 = jnp.float32
    whole = pl.BlockSpec(memory_space=pltpu.VMEM)
    hbm = pl.BlockSpec(memory_space=pltpu.HBM)
    return pl.pallas_call(
        functools.partial(segment_kernel, seqs, heads, key_dim, CHUNKS),
        in_specs=[hbm] * 7,
        out_specs=[whole, whole, whole],
        out_shape=[
            jax.ShapeDtypeStruct((devices * BLOCK_ROWS, val_dim), f32),
            jax.ShapeDtypeStruct((groups, key_dim), f32),
            jax.ShapeDtypeStruct((groups, val_dim), f32),
        ],
        scratch_shapes=[
            pltpu.VMEM((seqs, seg, model_width), jnp.bfloat16),
            pltpu.VMEM((model_width, width), jnp.bfloat16),
            pltpu.VMEM((model_width, width), jnp.bfloat16),
            pltpu.VMEM((seqs, model_width), jnp.bfloat16),
            pltpu.VMEM((1, model_width), f32),
            pltpu.VMEM((heads, key_dim), f32),
            pltpu.VMEM((seqs, heads, seg), f32),
            pltpu.VMEM((rows, width), f32),
            pltpu.VMEM((rows, width), f32),
            pltpu.VMEM((rows, 128), f32),
            pltpu.VMEM((groups, key_dim, val_dim), f32),
            pltpu.VMEM((256, 128), f32),
            pltpu.VMEM((seqs * seg, width), f32),
            pltpu.VMEM((128, 128), f32),
            pltpu.SemaphoreType.DMA((4, max(4, len(CHUNKS)))),
        ],
        compiler_params=pltpu.CompilerParams(vmem_limit_bytes=VMEM_MIB * 2**20),
        name="segment",
    )(
        *(pltpu.with_memory_space_constraint(x, pltpu.HBM) for x in (
            tokens, new_tokens, gain_row, w_forget, w_value, gap, shift_rows))
    )


def local(tokens, new_tokens, in_gain, w_forget, w_value, gap, decay_shift, query, out_gain):
    seqs, seg, model_width = tokens.shape
    heads, key_dim = gap.shape
    val_dim = out_gain.shape[1]
    devices = lax.axis_size("sp")
    per = key_dim // devices
    groups = seqs * heads
    whole = pl.BlockSpec(memory_space=pltpu.VMEM)
    f32 = jnp.float32
    buf, new_key, new_values = segments(
        tokens, new_tokens, in_gain.reshape(1, model_width), w_forget, w_value, gap,
        jnp.transpose(decay_shift, (0, 2, 1)))
    got = lax.all_to_all(
        buf.reshape(devices, BLOCK_ROWS, 1, val_dim), "sp", 0, 0, tiled=True
    ).reshape(devices * BLOCK_ROWS, val_dim)
    state, part = pl.pallas_call(
        functools.partial(settle_kernel, devices, per),
        in_specs=[whole, whole, whole, whole],
        out_specs=[whole, whole],
        out_shape=[
            jax.ShapeDtypeStruct((STATE_ROWS, val_dim), jnp.bfloat16),
            jax.ShapeDtypeStruct((devices * groups, val_dim), f32),
        ],
        scratch_shapes=[pltpu.VMEM((STATE_ROWS, val_dim), f32)],
        compiler_params=pltpu.CompilerParams(vmem_limit_bytes=8 * 2**20),
        name="settle",
    )(got, new_key, new_values, query)
    everything = lax.all_to_all(
        part.reshape(devices, groups, val_dim), "sp", 0, 0, tiled=True
    ).reshape(devices * groups, val_dim)
    read, cache = pl.pallas_call(
        functools.partial(read_kernel, devices),
        in_specs=[whole, whole, whole],
        out_specs=[whole, whole],
        out_shape=[
            jax.ShapeDtypeStruct((seqs, heads, val_dim), f32),
            jax.ShapeDtypeStruct((STATE_ROWS, val_dim), jnp.bfloat16),
        ],
        compiler_params=pltpu.CompilerParams(vmem_limit_bytes=8 * 2**20),
        name="read",
    )(everything, out_gain, state)
    return (cache.reshape(seqs, heads, per, val_dim), read)


def solution(mesh):
    return jax.shard_map(
        local,
        mesh=mesh,
        in_specs=(
            P("gr", "sp", None),
            P("gr", None),
            P(),
            P(None, "tp"),
            P(None, "tp"),
            P("tp", None),
            P("gr", "sp", "tp"),
            P("gr", "tp", "sp"),
            P("tp", None),
        ),
        out_specs=(P("gr", "tp", "sp", None), P("gr", "tp", None)),
        check_vma=False,
    )
```

```python
import functools

import jax
import jax.numpy as jnp
from jax import lax
from jax.experimental import pallas as pl
from jax.experimental.pallas import tpu as pltpu
from jax.sharding import PartitionSpec as P

epsilon = 1e-06

STATE_ROWS = 32
BLOCK_ROWS = 33
CHUNKS = (512,) * 8
VMEM_MIB = 48


def segment_kernel(
    seqs, heads, key_dim, chunks,
    tok_hbm, new_hbm, gain_hbm, wf_hbm, wv_hbm, gap_hbm, shift_hbm,
    buf_ref, nk_ref, nv_ref,
    tok_ref, wf_ref, wv_ref, new_ref, gain_ref, gap_ref, shift_ref, accf, accv, ssq, pieces, shift_cols, shift_wide, total_cols, sems,
):
    seg = tok_ref.shape[1]
    model_width = tok_ref.shape[2]
    rows = seqs * seg
    pad = accf.shape[0] - rows
    groups = seqs * heads
    rank = BLOCK_ROWS
    per = STATE_ROWS // groups
    devices = key_dim // per

    small = [
        pltpu.make_async_copy(source, target, sems.at[3, n])
        for n, (source, target) in enumerate(
            ((new_hbm, new_ref), (gain_hbm, gain_ref), (gap_hbm, gap_ref),
             (shift_hbm, shift_ref)))
    ]
    copies = []
    start = 0
    for n, size in enumerate(chunks):
        cols = slice(start, start + size)
        trio = [
            pltpu.make_async_copy(wf_hbm.at[cols, :], wf_ref.at[cols, :], sems.at[0, n]),
            pltpu.make_async_copy(wv_hbm.at[cols, :], wv_ref.at[cols, :], sems.at[1, n]),
            pltpu.make_async_copy(tok_hbm.at[:, :, cols], tok_ref.at[:, :, cols], sems.at[2, n]),
        ]
        for copy in trio:
            copy.start()
        if n == 0:
            for copy in small:
                copy.start()
        copies.append((cols, trio))
        start += size
    for copy in small:
        copy.wait()
    shift_rows = jnp.concatenate(
        [shift_ref[s] for s in range(seqs)]
        + [jnp.zeros((128 - groups, seg), jnp.float32)], axis=0)
    shift_rows = jnp.concatenate(
        [shift_rows, jnp.zeros((128, 256 - seg), jnp.float32)], axis=1)
    shift_cols[...] = shift_rows.T

    widened = [[] for _ in chunks]
    for s in range(seqs):
        widened[min(s + 2, len(chunks) - 1)].append(s)
    for n, (cols, trio) in enumerate(copies):
        for copy in trio:
            copy.wait()
        wide = tok_ref[:, :, cols].reshape(rows, chunks[n]).astype(jnp.float32)
        new = new_ref[:, cols].astype(jnp.float32)
        new = jnp.concatenate([new, jnp.zeros((pad - seqs, chunks[n]), jnp.float32)], axis=0)
        wide = jnp.concatenate([wide, new], axis=0)
        squares = wide * wide
        part = squares[:, 0:128]
        for c in range(1, chunks[n] // 128):
            part = part + squares[:, c * 128 : (c + 1) * 128]
        x = (wide * gain_ref[:, cols]).astype(jnp.bfloat16)
        yf = jnp.dot(x, wf_ref[cols, :], preferred_element_type=jnp.float32)
        yv = jnp.dot(x, wv_ref[cols, :], preferred_element_type=jnp.float32)
        if n == 0:
            accf[...] = yf
            accv[...] = yv
            ssq[...] = part
        else:
            accf[...] += yf
            accv[...] += yv
            ssq[...] += part
        for s in widened[n]:
            for h in range(heads):
                group = s * heads + h
                shift_wide[s * seg : (s + 1) * seg, h * key_dim : (h + 1) * key_dim] = (
                    jnp.broadcast_to(shift_cols[0:seg, group : group + 1], (seg, key_dim)))

    gap_row = jnp.concatenate([gap_ref[h : h + 1, :] for h in range(heads)], axis=1)
    ti = lax.broadcasted_iota(jnp.int32, (seg, seg), 0)
    tj = lax.broadcasted_iota(jnp.int32, (seg, seg), 1)
    later = (tj > ti).astype(jnp.float32).astype(jnp.bfloat16)
    total_rows = []
    gated = []
    for s in range(seqs):
        here = slice(s * seg, (s + 1) * seg)
        scale = lax.rsqrt(
            jnp.sum(ssq[here, :], axis=1, keepdims=True) / model_width + epsilon)
        key_gate = gap_row * jax.nn.sigmoid(-(accf[here, :] * scale))
        log_forget = jnp.log1p(-key_gate) + shift_wide[here, :]
        high = log_forget.astype(jnp.bfloat16)
        low = (log_forget - high.astype(jnp.float32)).astype(jnp.bfloat16)
        within = jnp.dot(later, high, preferred_element_type=jnp.float32)
        within = within + jnp.dot(later, low, preferred_element_type=jnp.float32)
        weights = (key_gate * jnp.exp(within)).astype(jnp.bfloat16)
        values = (accv[here, :] * scale).astype(jnp.bfloat16)
        total = jnp.sum(log_forget, axis=0, keepdims=True)
        for h in range(heads):
            lanes = slice(h * key_dim, (h + 1) * key_dim)
            group = s * heads + h
            total_rows.append(total[:, lanes])
            gated.append((weights[:, lanes], values[:, lanes]))
    for group in range(groups):
        pieces[group] = lax.dot_general(
            *gated[group], (((0,), (0,)), ((), ())), preferred_element_type=jnp.float32)
    for group in range(groups):
        for i in range(per):
            buf_ref[pl.ds(i * groups + group, devices, stride=rank), :] = (
                pieces[group, pl.ds(i, devices, stride=per), :])
    totals = jnp.concatenate(
        total_rows + [jnp.zeros((128 - groups, key_dim), jnp.float32)], axis=0)
    total_cols[...] = totals.T
    packed = total_cols[pl.ds(0, devices, stride=per), :]
    for i in range(1, per):
        packed = packed + pltpu.roll(
            total_cols[pl.ds(i, devices, stride=per), :], i * groups, 1)
    buf_ref[pl.ds(STATE_ROWS, devices, stride=rank), :] = packed
    for extra in range(STATE_ROWS + 1, rank):
        buf_ref[pl.ds(extra, devices, stride=rank), :] = jnp.zeros_like(packed)

    last = slice(rows, rows + pad)
    scale = lax.rsqrt(
        jnp.sum(ssq[last, :], axis=1, keepdims=True) / model_width + epsilon)
    new_key = gap_row * jax.nn.sigmoid(-(accf[last, :] * scale))
    new_values = (accv[last, :] * scale).astype(jnp.bfloat16).astype(jnp.float32)
    for h in range(heads):
        lanes = slice(h * key_dim, (h + 1) * key_dim)
        nk_ref[pl.ds(h, seqs, stride=heads), :] = new_key[0:seqs, lanes]
        nv_ref[pl.ds(h, seqs, stride=heads), :] = new_values[0:seqs, lanes]


def settle_kernel(
    devices, per,
    got_ref, nk_ref, nv_ref, query_ref,
    cache_ref, part_ref, state_ref,
):
    groups = nk_ref.shape[0]
    totals = got_ref[pl.ds(STATE_ROWS, devices, stride=BLOCK_ROWS), :]
    own = lax.broadcasted_iota(jnp.int32, (devices, devices), 0)
    other = lax.broadcasted_iota(jnp.int32, (devices, devices), 1)
    after = (other > own).astype(jnp.float32).astype(jnp.bfloat16)
    later = jnp.zeros_like(totals)
    for _ in range(3):
        part = totals.astype(jnp.bfloat16)
        later = later + jnp.dot(after, part, preferred_element_type=jnp.float32)
        totals = totals - part.astype(jnp.float32)
    factor = jnp.exp(later).T[0:STATE_ROWS]
    lane = lax.broadcasted_iota(jnp.int32, (groups, 128), 1)
    first = lax.axis_index("sp") * per
    query = jnp.concatenate(
        [query_ref[s].astype(jnp.float32) for s in range(query_ref.shape[0])], axis=0)
    part = jnp.zeros((groups, 128), jnp.float32)
    for i in range(per):
        base = i * groups
        state = factor[base : base + groups, 0:1] * got_ref[base : base + groups, :]
        for g in range(1, devices):
            start = g * BLOCK_ROWS + base
            state = state + factor[base : base + groups, g : g + 1] * got_ref[
                start : start + groups, :]
        state_ref[pl.ds(i, groups, stride=per), :] = state
        new_key = jnp.sum(
            jnp.where(lane == first + i, nk_ref[...], 0.0), axis=1, keepdims=True)
        updated = (1.0 - new_key) * state + new_key * nv_ref[...]
        part = part + query[:, i : i + 1] * updated
    cache_ref[...] = state_ref[...].astype(jnp.bfloat16)
    for d in range(devices):
        part_ref[d * groups : (d + 1) * groups, :] = part


def read_kernel(devices, got_ref, gain_ref, state_ref, read_ref, cache_ref):
    seqs, heads, val_dim = read_ref.shape
    cache_ref[...] = state_ref[...]
    groups = seqs * heads
    sums = [got_ref[d * groups : (d + 1) * groups, :] for d in range(devices)]
    while len(sums) > 1:
        sums = [a + b for a, b in zip(sums[0::2], sums[1::2])] + sums[len(sums) // 2 * 2 :]
    raw = sums[0]
    gain = jnp.concatenate([gain_ref[...]] * seqs, axis=0)
    mean = jnp.sum(raw * raw, axis=1, keepdims=True) / val_dim
    out = raw * lax.rsqrt(mean + epsilon) * gain
    for s in range(seqs):
        read_ref[s] = out[s * heads : (s + 1) * heads, :]


def segments(tokens, new_tokens, gain_row, w_forget, w_value, gap, shift_rows):
    seqs, seg, model_width = tokens.shape
    heads, key_dim = gap.shape
    width = w_forget.shape[1]
    val_dim = width // heads
    groups = seqs * heads
    devices = key_dim * groups // STATE_ROWS
    rows = seqs * seg + 16
    f32 = jnp.float32
    whole = pl.BlockSpec(memory_space=pltpu.VMEM)
    hbm = pl.BlockSpec(memory_space=pltpu.HBM)
    return pl.pallas_call(
        functools.partial(segment_kernel, seqs, heads, key_dim, CHUNKS),
        in_specs=[hbm] * 7,
        out_specs=[whole, whole, whole],
        out_shape=[
            jax.ShapeDtypeStruct((devices * BLOCK_ROWS, val_dim), f32),
            jax.ShapeDtypeStruct((groups, key_dim), f32),
            jax.ShapeDtypeStruct((groups, val_dim), f32),
        ],
        scratch_shapes=[
            pltpu.VMEM((seqs, seg, model_width), jnp.bfloat16),
            pltpu.VMEM((model_width, width), jnp.bfloat16),
            pltpu.VMEM((model_width, width), jnp.bfloat16),
            pltpu.VMEM((seqs, model_width), jnp.bfloat16),
            pltpu.VMEM((1, model_width), f32),
            pltpu.VMEM((heads, key_dim), f32),
            pltpu.VMEM((seqs, heads, seg), f32),
            pltpu.VMEM((rows, width), f32),
            pltpu.VMEM((rows, width), f32),
            pltpu.VMEM((rows, 128), f32),
            pltpu.VMEM((groups, key_dim, val_dim), f32),
            pltpu.VMEM((256, 128), f32),
            pltpu.VMEM((seqs * seg, width), f32),
            pltpu.VMEM((128, 128), f32),
            pltpu.SemaphoreType.DMA((4, max(4, len(CHUNKS)))),
        ],
        compiler_params=pltpu.CompilerParams(vmem_limit_bytes=VMEM_MIB * 2**20),
        name="segment",
    )(
        *(pltpu.with_memory_space_constraint(x, pltpu.HBM) for x in (
            tokens, new_tokens, gain_row, w_forget, w_value, gap, shift_rows))
    )


def local(tokens, new_tokens, in_gain, w_forget, w_value, gap, decay_shift, query, out_gain):
    seqs, seg, model_width = tokens.shape
    heads, key_dim = gap.shape
    val_dim = out_gain.shape[1]
    devices = lax.axis_size("sp")
    per = key_dim // devices
    groups = seqs * heads
    whole = pl.BlockSpec(memory_space=pltpu.VMEM)
    f32 = jnp.float32
    buf, new_key, new_values = segments(
        tokens, new_tokens, in_gain.reshape(1, model_width), w_forget, w_value, gap,
        jnp.transpose(decay_shift, (0, 2, 1)))
    got = lax.all_to_all(
        buf.reshape(devices, BLOCK_ROWS, 1, val_dim), "sp", 0, 0, tiled=True
    ).reshape(devices * BLOCK_ROWS, val_dim)
    state, part = pl.pallas_call(
        functools.partial(settle_kernel, devices, per),
        in_specs=[whole, whole, whole, whole],
        out_specs=[whole, whole],
        out_shape=[
            jax.ShapeDtypeStruct((STATE_ROWS, val_dim), jnp.bfloat16),
            jax.ShapeDtypeStruct((devices * groups, val_dim), f32),
        ],
        scratch_shapes=[pltpu.VMEM((STATE_ROWS, val_dim), f32)],
        compiler_params=pltpu.CompilerParams(vmem_limit_bytes=8 * 2**20),
        name="settle",
    )(got, new_key, new_values, query)
    everything = lax.all_to_all(
        part.reshape(devices, groups, val_dim), "sp", 0, 0, tiled=True
    ).reshape(devices * groups, val_dim)
    read, cache = pl.pallas_call(
        functools.partial(read_kernel, devices),
        in_specs=[whole, whole, whole],
        out_specs=[whole, whole],
        out_shape=[
            jax.ShapeDtypeStruct((seqs, heads, val_dim), f32),
            jax.ShapeDtypeStruct((STATE_ROWS, val_dim), jnp.bfloat16),
        ],
        compiler_params=pltpu.CompilerParams(vmem_limit_bytes=8 * 2**20),
        name="read",
    )(everything, out_gain, state)
    return (cache.reshape(seqs, heads, per, val_dim), read)


def solution(mesh):
    return jax.shard_map(
        local,
        mesh=mesh,
        in_specs=(
            P("gr", "sp", None),
            P("gr", None),
            P(),
            P(None, "tp"),
            P(None, "tp"),
            P("tp", None),
            P("gr", "sp", "tp"),
            P("gr", "tp", "sp"),
            P("tp", None),
        ),
        out_specs=(P("gr", "tp", "sp", None), P("gr", "tp", None)),
        check_vma=False,
    )
```
